32 devices in a mesh: kv: 8 (over z, y), tp: 4 (over x, core).
Axes of the slice: x: 2, y: 2, z: 4, core: 2. Of those that a mesh axis runs over, the one named last changes fastest.
Arguments:
- tokens: bfloat16 [32, 4096], P(None, 'kv'), may hold values from -8 to 8, as said below
- attn_gain: float32 [4096], P('kv'), may hold values from 0.1 to 1.9
- query_weight: bfloat16 [4096, 1024], P('kv', 'tp'), may hold values from -0.09375 to 0.09375
- key_weight: bfloat16 [4096, 1024], P('kv', 'tp'), may hold values from -0.09375 to 0.09375
- value_weight: bfloat16 [4096, 2048], P('kv', 'tp'), may hold values from -0.09375 to 0.09375
- outgate_weight: bfloat16 [4096, 2048], P('kv', 'tp'), may hold values from -0.09375 to 0.09375
- code_weight: bfloat16 [4096, 16], P('kv'), may hold values from -0.09375 to 0.09375
- decay_weight: bfloat16 [16, 1024], P(None, 'tp'), may hold values from -6 to 6
- decay_bias: float32 [1024], P('tp'), may hold values from -4 to 2
- head_gain: float32 [256], replicated, may hold values from 0.1 to 1.9
- key_cache: bfloat16 [32, 64, 8, 128], P('kv', None, 'tp'), may hold values from -6 to 6
- value_cache: bfloat16 [32, 64, 8, 256], P('kv', None, 'tp'), may hold values from -6 to 6
- decay_cache: float32 [32, 64, 8, 128], P('kv', None, 'tp'), may hold values from -1.1 to 0
- carried_state: float32 [32, 8, 128, 256], P('kv', 'tp'), may hold values from -24 to 24
- lengths: int32 [32], P('kv'), may hold values from 1 to 64, 832 in all
- output_weight: bfloat16 [2048, 4096], P('tp', 'kv'), may hold values from -0.125 to 0.125
- mlp_gain: float32 [4096], P('kv'), may hold values from 0.1 to 1.9
- gate_weight: bfloat16 [4096, 11008], P('kv', 'tp'), may hold values from -0.09375 to 0.09375
- up_weight: bfloat16 [4096, 11008], P('kv', 'tp'), may hold values from -0.09375 to 0.09375
- down_weight: bfloat16 [11008, 4096], P('tp', 'kv'), may hold values from -0.0546875 to 0.0546875
Outputs:
- layer_out: bfloat16 [32, 4096], P(None, 'kv')
- new_keys: bfloat16 [32, 8, 128], P('kv', 'tp')
- new_values: bfloat16 [32, 8, 256], P('kv', 'tp')
The draws below stay inside these ranges and needn't reach their ends.
Inputs may be any that keep to these rules, and one draw needn't show every extreme that they name: `tokens`: the features of a row have unlike scales. Sequence b's new token comes right after its lengths[b] live positions; positions from lengths[b] on take no part.
All inputs are finite; a program needn't handle non-finite values. No bound on the sum of `lengths` on one device may be relied on, other than what follows from the above.
Results may differ from the reference program's by a relative error of at most 0.025.
Values may be sent and summed in bfloat16 or wider, within the bound.
A program may use at most 64 MiB of HBM per device.

```python
import math
import jax
import jax.numpy as jnp
import numpy as np
from jax import lax

WIDTH = 4096
HEAD_COUNT = 8
KEY_DIM = 128
VALUE_DIM = 256
KEY_WIDTH = 1024
VALUE_WIDTH = 2048
GATE_RANK = 16
MLP_WIDTH = 11008
BLOCK_SPAN = 64
BATCH_TOTAL = 32
N_TP = 4


def draw_tokens(key, part):
    base_key, rough_key = jax.random.split(jax.random.fold_in(key, 11), 2)
    column = jnp.arange(WIDTH, dtype=jnp.float32) / WIDTH
    jaggedness = jax.random.uniform(rough_key, (WIDTH,), jnp.float32, 0.5, 2.0)
    scales = 10.0 ** (column - 0.75) * jaggedness
    values = jax.random.normal(base_key, (BATCH_TOTAL, WIDTH), jnp.float32) * scales[None, :]
    return jnp.clip(values, -8.0, 8.0).astype(jnp.bfloat16)


def draw_decay_cache(key, part):
    random_split_keys = jax.random.split(jax.random.fold_in(key, 23), 5)
    slowest = 0.002
    fastest = 0.12
    channel_frequencies = jnp.exp(jax.random.uniform(random_split_keys[0], (1, 1, HEAD_COUNT, KEY_DIM), jnp.float32, math.log(slowest), math.log(fastest)))
    sequence_wise = jnp.exp(jax.random.uniform(random_split_keys[1], (BATCH_TOTAL, 1, 1, 1), jnp.float32, math.log(0.5), math.log(2.0)))
    jaggedness = jax.random.uniform(random_split_keys[2], (BATCH_TOTAL, BLOCK_SPAN, HEAD_COUNT, KEY_DIM), jnp.float32, 0.5, 1.5)
    spike_events = jax.random.randint(random_split_keys[3], (BATCH_TOTAL, BLOCK_SPAN, 1, 1), 0, BLOCK_SPAN) < 3
    spike_removal = jax.random.uniform(random_split_keys[4], (BATCH_TOTAL, BLOCK_SPAN, HEAD_COUNT, 1), jnp.float32, math.log(0.5), math.log(0.8))
    return -channel_frequencies * sequence_wise * jaggedness + jnp.where(spike_events, spike_removal, 0.0)


def levels(stream_key, extent, shards, smallest, top_value):
    def one(dim, blocks):
        heights = jax.random.uniform(jax.random.fold_in(jax.random.fold_in(stream_key, 6), dim), (blocks,), jnp.float32, smallest / len(shards), top_value / len(shards))
        return jnp.repeat(jnp.exp(heights), extent[dim] // blocks).reshape((-1,) + (1,) * (len(extent) - dim - 1))

    level = one(*shards[0])
    for cut in shards[1:]:
        level = level * one(*cut)
    return level


def split_up(amount, total, limit, slope):
    loads = [(1 << 20) // math.isqrt(grade ** slope) + 1 for grade in range(2, amount + 1)]
    surplus, given = total - limit - (amount - 1), [1] * (amount - 1)
    while surplus > 0:
        candidates = [i for i in range(amount - 1) if given[i] < limit]
        whole, remaining = sum([loads[i] for i in candidates]), surplus
        for i in candidates:
            more = min(limit - given[i], max(1, remaining * loads[i] // whole), surplus)
            given[i] = given[i] + more
            surplus = surplus - more
    return np.array([limit] + given)


def ragged_sizes(own_key, count, total, limit, slope):
    if count == 2:
        one = jax.random.randint(own_key, (), max(1, total - limit), min(limit, total - 1) + 1)
        return jnp.stack([one, total - one])
    sizes = jnp.asarray(split_up(count, total, limit, slope), jnp.int32)
    couples = (count - 1) // 2
    source_of, taker = sizes[1:1 + 2 * couples:2], sizes[2:2 + 2 * couples:2]
    room = jnp.minimum(source_of - 1, limit - taker)
    shifted = jax.random.randint(jax.random.fold_in(own_key, 1), (couples,), 0, 1 << 20) % (room + 1)
    sizes = sizes.at[1:1 + 2 * couples:2].set(source_of - shifted).at[2:2 + 2 * couples:2].set(taker + shifted)
    return sizes[jax.random.permutation(jax.random.fold_in(own_key, 2), count)]


def scatter_about(own_key, dims, scale, most, pieces=(), kind=jnp.bfloat16):
    result = jax.random.normal(own_key, dims, jnp.float32) * scale
    if len(pieces) > 0:
        result = levels(own_key, dims, pieces, -0.22, 0.18) * result
    return jnp.clip(result, min=-most, max=most).astype(kind)


def setup_inputs(seed: int = 0) -> dict:
    streams_of = jax.random.split(jax.random.key(seed), 21)
    return {
        "tokens": draw_tokens(jax.random.fold_in(streams_of[20], 71), 0),
        "attn_gain": jnp.clip(1.0 + 0.18 * jax.random.normal(streams_of[1], (WIDTH,), jnp.float32), 0.1, 1.9),
        "query_weight": scatter_about(streams_of[2], (WIDTH, KEY_WIDTH), WIDTH ** -0.5, 0.09375, ((0, 8), (1, 4))),
        "key_weight": scatter_about(streams_of[3], (WIDTH, KEY_WIDTH), WIDTH ** -0.5, 0.09375, ((0, 8), (1, 4))),
        "value_weight": scatter_about(streams_of[4], (WIDTH, VALUE_WIDTH), WIDTH ** -0.5, 0.09375, ((0, 8), (1, 4))),
        "outgate_weight": scatter_about(streams_of[5], (WIDTH, VALUE_WIDTH), WIDTH ** -0.5, 0.09375, ((0, 8), (1, 4))),
        "code_weight": scatter_about(streams_of[6], (WIDTH, GATE_RANK), WIDTH ** -0.5, 0.09375, ((0, 8),)),
        "decay_weight": scatter_about(streams_of[7], (GATE_RANK, KEY_WIDTH), 1 ** -0.5, 6.0, ((1, 4),)),
        "decay_bias": jnp.clip(-4.0 + 6.0 * jax.random.uniform(streams_of[8], (KEY_WIDTH,), jnp.float32) ** levels(streams_of[8], (KEY_WIDTH,), ((0, 4),), -0.2, 0.2), -4.0, 2.0),
        "head_gain": jnp.clip(1.0 + 0.18 * jax.random.normal(streams_of[9], (VALUE_DIM,), jnp.float32), 0.1, 1.9),
        "key_cache": scatter_about(streams_of[10], (BATCH_TOTAL, BLOCK_SPAN, HEAD_COUNT, KEY_DIM), 1.0, 6.0, ((0, 8), (2, 4))),
        "value_cache": scatter_about(streams_of[11], (BATCH_TOTAL, BLOCK_SPAN, HEAD_COUNT, VALUE_DIM), 1.0, 6.0, ((0, 8), (2, 4))),
        "decay_cache": draw_decay_cache(jax.random.fold_in(streams_of[20], 71), 0),
        "carried_state": scatter_about(streams_of[13], (BATCH_TOTAL, HEAD_COUNT, KEY_DIM, VALUE_DIM), 4.0, 24.0, ((0, 8), (1, 4)), jnp.float32),
        "lengths": ragged_sizes(streams_of[14], BATCH_TOTAL, BATCH_TOTAL * (13 * BLOCK_SPAN // 32), BLOCK_SPAN, 2).astype(jnp.int32),
        "output_weight": scatter_about(streams_of[15], (VALUE_WIDTH, WIDTH), VALUE_WIDTH ** -0.5, 0.125, ((0, 4), (1, 8))),
        "mlp_gain": jnp.clip(1.0 + 0.18 * jax.random.normal(streams_of[16], (WIDTH,), jnp.float32), 0.1, 1.9),
        "gate_weight": scatter_about(streams_of[17], (WIDTH, MLP_WIDTH), WIDTH ** -0.5, 0.09375, ((0, 8), (1, 4))),
        "up_weight": scatter_about(streams_of[18], (WIDTH, MLP_WIDTH), WIDTH ** -0.5, 0.09375, ((0, 8), (1, 4))),
        "down_weight": scatter_about(streams_of[19], (MLP_WIDTH, WIDTH), MLP_WIDTH ** -0.5, 0.0546875, ((0, 4), (1, 8))),
    }


EPS = 1e-06
GATE_TEMP = 16.0

def block_attention(queries, new_keys, new_values, new_decay, key_cache, value_cache, decay_cache, carried_state, lengths):
    positions = jnp.arange(key_cache.shape[1], dtype=jnp.int32)
    live_mask = positions[None, :] < lengths[:, None]
    kept_decay = jnp.where(live_mask[:, :, None, None], decay_cache, jnp.zeros_like(decay_cache))
    later_sum = lax.cumsum(kept_decay, axis=1, reverse=True) - kept_decay
    total_decay = lax.optimization_barrier(jnp.sum(kept_decay, axis=1))
    decayed = queries.astype(jnp.float32) * jnp.exp(new_decay)
    carried = jnp.einsum('bhd,bhde->bhe', decayed * jnp.exp(total_decay), carried_state, precision=lax.Precision.HIGHEST)
    keyed_cache = key_cache.astype(jnp.float32) * jnp.exp(later_sum)
    scores = jnp.einsum('bhd,bshd->bhs', decayed, keyed_cache, precision=lax.Precision.HIGHEST)
    scores = jnp.where(live_mask[:, None, :], scores, jnp.zeros_like(scores)).astype(jnp.bfloat16)
    within = jnp.einsum('bhs,bshe->bhe', scores.astype(jnp.float32), value_cache.astype(jnp.float32))
    own_score = lax.optimization_barrier(jnp.sum(queries.astype(jnp.float32) * new_keys.astype(jnp.float32), axis=-1))
    return carried + within + own_score[..., None] * new_values.astype(jnp.float32)

def summed_by_group(left, weight, groups):
    row_count, inner_dim = left.shape
    group_parts = jnp.einsum('bni,nid->bnd', left.reshape(row_count, groups, inner_dim // groups).astype(jnp.float32), weight.reshape(groups, inner_dim // groups, weight.shape[1]).astype(jnp.float32))
    group_parts = lax.optimization_barrier(group_parts.astype(jnp.bfloat16))
    return lax.optimization_barrier(jnp.sum(group_parts.astype(jnp.float32), axis=1))

def reference(tokens, attn_gain, query_weight, key_weight, value_weight, outgate_weight, code_weight, decay_weight, decay_bias, head_gain, key_cache, value_cache, decay_cache, carried_state, lengths, output_weight, mlp_gain, gate_weight, up_weight, down_weight):
    token_f = tokens.astype(jnp.float32)
    scaled = (token_f * attn_gain[None, :]).astype(jnp.bfloat16)
    inv_rms = lax.rsqrt(lax.optimization_barrier(jnp.mean(token_f * token_f, axis=1, keepdims=True)) + EPS)

    def project(weight):
        return jnp.dot(scaled, weight, preferred_element_type=jnp.float32) * inv_rms
    queries = (project(query_weight) * KEY_DIM ** (-0.5)).astype(jnp.bfloat16).reshape(BATCH_TOTAL, HEAD_COUNT, KEY_DIM)
    new_keys = project(key_weight).astype(jnp.bfloat16).reshape(BATCH_TOTAL, HEAD_COUNT, KEY_DIM)
    new_values = project(value_weight).astype(jnp.bfloat16).reshape(BATCH_TOTAL, HEAD_COUNT, VALUE_DIM)
    out_gate = project(outgate_weight).astype(jnp.bfloat16).reshape(BATCH_TOTAL, HEAD_COUNT, VALUE_DIM)
    gate_code = project(code_weight).astype(jnp.bfloat16)
    pre_gate = jnp.dot(gate_code, decay_weight, preferred_element_type=jnp.float32) + decay_bias[None, :]
    new_decay = (jax.nn.log_sigmoid(pre_gate) / GATE_TEMP).reshape(BATCH_TOTAL, HEAD_COUNT, KEY_DIM)
    mixed_heads = block_attention(queries, new_keys, new_values, new_decay, key_cache, value_cache, decay_cache, carried_state, lengths)
    normed = mixed_heads * lax.rsqrt(lax.optimization_barrier(jnp.mean(mixed_heads * mixed_heads, axis=-1, keepdims=True)) + EPS) * head_gain
    heads_out = (normed * jax.nn.silu(out_gate.astype(jnp.float32))).astype(jnp.bfloat16).reshape(BATCH_TOTAL, HEAD_COUNT * VALUE_DIM)
    attended = summed_by_group(heads_out, output_weight, N_TP)
    middle = (token_f + attended).astype(jnp.bfloat16)
    mid_f = middle.astype(jnp.float32)
    scaled_mid = (mid_f * mlp_gain[None, :]).astype(jnp.bfloat16)
    inv_mid = lax.rsqrt(lax.optimization_barrier(jnp.mean(mid_f * mid_f, axis=1, keepdims=True)) + EPS)
    gate_act = jnp.dot(scaled_mid, gate_weight, preferred_element_type=jnp.float32) * inv_mid
    up_act = jnp.dot(scaled_mid, up_weight, preferred_element_type=jnp.float32) * inv_mid
    hidden = (jax.nn.silu(gate_act) * up_act).astype(jnp.bfloat16)
    lifted = summed_by_group(hidden, down_weight, N_TP)
    layer_out = (mid_f + lifted).astype(jnp.bfloat16)
    return (layer_out, new_keys, new_values)
```

```python
import functools

import jax
import jax.numpy as jnp
from jax import lax
from jax.experimental import pallas as pl
from jax.experimental.pallas import tpu as pltpu
from jax.sharding import PartitionSpec as P

EPS = 1e-06
GATE_TEMP = 16.0
LANES = 128
F32 = jnp.float32
BF16 = jnp.bfloat16


def split_sum(column):
    high = column.astype(BF16).astype(F32)
    return high, column - high


def dot(left, right):
    return jnp.dot(left, right, preferred_element_type=F32)


def tiles_of(total, step):
    return [(start, min(step, total - start)) for start in range(0, total, step)]


def layer_kernel(
    n_kv,
    n_tp,
    width,
    tokens_h,
    attn_gain_h,
    wq_h,
    wk_h,
    wv_h,
    wg_h,
    wc_h,
    dw_h,
    db_h,
    head_gain_h,
    key_h,
    value_h,
    decay_h,
    state_h,
    lengths_s,
    wo_h,
    mlp_gain_h,
    gate_h,
    up_h,
    down_h,
    out_ref,
    nk_ref,
    nv_ref,
    tokens,
    attn_gain,
    wq,
    wk,
    wv,
    wg,
    wc,
    dw,
    db,
    head_gain,
    key,
    value,
    decay,
    state,
    wo,
    mlp_gain,
    gate,
    up,
    down,
    proj,
    proj_send,
    proj_recv,
    keyed,
    total_exp,
    decayed3,
    keys3,
    values3,
    mixed,
    heads,
    heads_all,
    attended,
    mlp_acc,
    mlp_send,
    mlp_recv,
    hidden,
    hidden_all,
    lifted,
    load_sem,
    send_a,
    recv_a,
    send_b,
    recv_b,
    send_c,
    recv_c,
    send_d,
    recv_d,
    send_e,
    recv_e,
    send_f,
    recv_f,
):
    kv_me = lax.axis_index("kv")
    tp_me = lax.axis_index("tp")
    rows, feats = tokens.shape
    seqs, span, heads_here, key_dim = key.shape
    value_dim = value.shape[3]
    kw, vw = heads_here * key_dim, heads_here * value_dim
    rank = wc.shape[1]
    units = gate.shape[1]
    padded = hidden.shape[1]

    loads = {}
    pairs = [
        ("tokens", tokens_h, tokens),
        ("attn_gain", attn_gain_h, attn_gain),
        ("wc", wc_h, wc),
        ("wq", wq_h, wq),
        ("wk", wk_h, wk),
        ("wv", wv_h, wv),
        ("wg", wg_h, wg),
        ("decay", decay_h, decay),
        ("key", key_h, key),
        ("dw", dw_h, dw.at[pl.ds(0, rank)]),
        ("db", db_h, db),
        ("head_gain", head_gain_h, head_gain),
        ("state", state_h, state),
        ("value", value_h, value),
        ("wo", wo_h, wo),
        ("mlp_gain", mlp_gain_h, mlp_gain),
        ("gate", gate_h, gate),
        ("up", up_h, up),
        ("down", down_h, down.at[pl.ds(0, units)]),
    ]
    for place, (name, source, target) in enumerate(pairs):
        loads[name] = pltpu.make_async_copy(source, target, load_sem.at[place])
        loads[name].start()

    barrier = pltpu.get_barrier_semaphore()
    for off in range(1, n_kv):
        pl.semaphore_signal(
            barrier,
            inc=1,
            device_id={"kv": lax.rem(kv_me + off, n_kv)},
            device_id_type=pl.DeviceIdType.MESH,
        )
    for off in range(1, n_tp):
        pl.semaphore_signal(
            barrier,
            inc=1,
            device_id={"tp": lax.rem(tp_me + off, n_tp)},
            device_id_type=pl.DeviceIdType.MESH,
        )

    def exchange(axis, me, count, source, target, sends, recvs):
        started = []
        for off in range(count - 1, 0, -1):
            p = lax.rem(me + off, count)
            copy = pltpu.make_async_remote_copy(
                src_ref=source(p),
                dst_ref=target.at[me],
                send_sem=sends.at[off],
                recv_sem=recvs.at[me],
                device_id={axis: p},
                device_id_type=pl.DeviceIdType.MESH,
            )
            copy.start()
            started.append(copy)
        return started

    def await_arrivals(me, count, target, recvs):
        for off in range(1, count):
            p = lax.rem(me + off, count)
            pltpu.make_async_copy(target.at[p], target.at[p], recvs.at[p]).wait()

    pending = []

    base_misc = 2 * kw + 2 * vw
    for name in ("tokens", "attn_gain", "wc"):
        loads[name].wait()
    token_f = tokens[...].astype(F32)
    scaled = (token_f * attn_gain[...]).astype(BF16)
    proj[:, base_misc:] = jnp.zeros((rows, LANES), F32)
    proj[:, base_misc : base_misc + rank] = dot(scaled, wc[...])
    high, low = split_sum(jnp.sum(token_f * token_f, axis=1, keepdims=True))
    proj[:, base_misc + rank : base_misc + rank + 1] = high
    proj[:, base_misc + rank + 1 : base_misc + rank + 2] = low
    base = 0
    for name, weight in (("wq", wq), ("wk", wk), ("wv", wv), ("wg", wg)):
        loads[name].wait()
        for start, size in tiles_of(weight.shape[1], 256):
            proj[:, base + start : base + start + size] = dot(
                scaled, weight[:, start : start + size]
            )
        base += weight.shape[1]
    for p in range(n_kv):
        proj_send[p] = proj[p * seqs : (p + 1) * seqs, :].astype(BF16)
    pl.semaphore_wait(barrier, n_kv + n_tp - 2)
    pending += exchange("kv", kv_me, n_kv, lambda p: proj_send.at[p], proj_recv, send_a, recv_a)
    proj_recv[kv_me] = proj_send[kv_me]

    dw[rank:, :] = jnp.zeros((dw.shape[0] - rank, dw.shape[1]), BF16)
    if padded > units:
        down[units:, :] = jnp.zeros((padded - units, down.shape[1]), BF16)
        hidden[:, units:] = jnp.zeros((rows, padded - units), F32)
    loads["decay"].wait()
    loads["key"].wait()
    positions = lax.broadcasted_iota(jnp.int32, (span, heads_here, key_dim), 0)
    for b in range(seqs):
        live = positions < lengths_s[b]
        kept = jnp.where(live, decay[b], 0.0)
        suffix = kept
        step = 1
        while step < span:
            suffix = suffix + jnp.concatenate(
                [suffix[step:], jnp.zeros((step, heads_here, key_dim), F32)], axis=0
            )
            step *= 2
        total_exp[b] = jnp.exp(suffix[0])
        later = jnp.concatenate([suffix[1:], jnp.zeros((1, heads_here, key_dim), F32)], axis=0)
        keyed[b] = jnp.where(live, key[b].astype(F32) * jnp.exp(later), 0.0)
    for name in ("dw", "db", "head_gain", "state", "value"):
        loads[name].wait()

    await_arrivals(kv_me, n_kv, proj_recv, recv_a)
    total = proj_recv[0].astype(F32)
    for p in range(1, n_kv):
        total = total + proj_recv[p].astype(F32)
    misc = total[:, base_misc:]
    squares = misc[:, rank : rank + 1] + misc[:, rank + 1 : rank + 2]
    inv_rms = lax.rsqrt(squares / width + EPS)
    queries = (total[:, :kw] * inv_rms * key_dim ** (-0.5)).astype(BF16).astype(F32)
    new_keys = (total[:, kw : 2 * kw] * inv_rms).astype(BF16).astype(F32)
    new_values = (total[:, 2 * kw : 2 * kw + vw] * inv_rms).astype(BF16).astype(F32)
    out_gate = (total[:, 2 * kw + vw : base_misc] * inv_rms).astype(BF16).astype(F32)
    code = (misc * inv_rms).astype(BF16)
    pre_gate = dot(code, dw[...]) + db[...]
    new_decay = (jnp.minimum(pre_gate, 0.0) - jnp.log1p(jnp.exp(-jnp.abs(pre_gate)))) / GATE_TEMP
    decayed = queries * jnp.exp(new_decay)
    for b in range(seqs):
        for h in range(heads_here):
            k_cols = slice(h * key_dim, (h + 1) * key_dim)
            v_cols = slice(h * value_dim, (h + 1) * value_dim)
            decayed3[b, h : h + 1, :] = decayed[b : b + 1, k_cols]
            keys3[b, h : h + 1, :] = new_keys[b : b + 1, k_cols]
            values3[b, h : h + 1, :] = new_values[b : b + 1, v_cols]
    nk_ref[...] = keys3[...].astype(BF16)
    nv_ref[...] = values3[...].astype(BF16)
    for b in range(seqs):
        d = decayed3[b]
        scores = jnp.sum(keyed[b] * d[None], axis=-1, keepdims=True)
        scores = scores.astype(BF16).astype(F32)
        within = jnp.sum(scores * value[b].astype(F32), axis=0)
        into_state = jnp.transpose(
            jnp.concatenate(
                [d * total_exp[b], jnp.zeros((8 - heads_here, key_dim), F32)], axis=0
            )
        )
        for h in range(heads_here):
            carried = jnp.sum(into_state[:, h : h + 1] * state[b, h], axis=0, keepdims=True)
            mixed[b : b + 1, h * value_dim : (h + 1) * value_dim] = carried + within[h : h + 1]
    for h in range(heads_here):
        k_cols = slice(h * key_dim, (h + 1) * key_dim)
        v_cols = slice(h * value_dim, (h + 1) * value_dim)
        own = jnp.sum(queries[:, k_cols] * new_keys[:, k_cols], axis=-1, keepdims=True)
        full = mixed[:, v_cols] + own * new_values[:, v_cols]
        norm = lax.rsqrt(jnp.mean(full * full, axis=-1, keepdims=True) + EPS)
        g = out_gate[:, v_cols]
        mixed[:, v_cols] = full * norm * head_gain[...] * (g / (1.0 + jnp.exp(-g)))
    heads_all[kv_me] = mixed[...].astype(BF16)
    pending += exchange(
        "kv", kv_me, n_kv, lambda p: heads_all.at[kv_me], heads_all, send_b, recv_b
    )

    loads["wo"].wait()
    loads["mlp_gain"].wait()
    await_arrivals(kv_me, n_kv, heads_all, recv_b)
    for p in range(n_kv):
        heads[p * seqs : (p + 1) * seqs, :] = heads_all[p].astype(F32)
    attended[tp_me] = dot(heads[...].astype(BF16), wo[...]).astype(BF16)
    pending += exchange(
        "tp", tp_me, n_tp, lambda p: attended.at[tp_me], attended, send_c, recv_c
    )
    loads["gate"].wait()
    await_arrivals(tp_me, n_tp, attended, recv_c)
    summed = attended[0].astype(F32)
    for p in range(1, n_tp):
        summed = summed + attended[p].astype(F32)
    mid_f = (token_f + summed).astype(BF16).astype(F32)
    scaled_mid = (mid_f * mlp_gain[...]).astype(BF16)

    for part, (name, weight) in enumerate((("gate", gate), ("up", up))):
        if part:
            loads[name].wait()
        else:
            mlp_acc[:, padded - LANES :] = jnp.zeros((rows, LANES), F32)
        for start, size in tiles_of(units, 256):
            mlp_acc[:, start : start + size] = dot(scaled_mid, weight[:, start : start + size])
        if part == 0:
            high, low = split_sum(jnp.sum(mid_f * mid_f, axis=1, keepdims=True))
            mlp_acc[:, units : units + 1] = high
            mlp_acc[:, units + 1 : units + 2] = low
        for p in range(n_kv):
            mlp_send[part, p] = mlp_acc[p * seqs : (p + 1) * seqs, :].astype(BF16)
        pending += exchange(
            "kv",
            kv_me,
            n_kv,
            lambda p, part=part: mlp_send.at[part, p],
            mlp_recv.at[part],
            send_d.at[part],
            recv_d.at[part],
        )
        mlp_recv[part, kv_me] = mlp_send[part, kv_me]
    sums = []
    for part in range(2):
        await_arrivals(kv_me, n_kv, mlp_recv.at[part], recv_d.at[part])
        total = mlp_recv[part, 0].astype(F32)
        for p in range(1, n_kv):
            total = total + mlp_recv[part, p].astype(F32)
        sums.append(total)
    squares = sums[0][:, units : units + 1] + sums[0][:, units + 1 : units + 2]
    inv_mid = lax.rsqrt(squares / width + EPS)
    g = sums[0] * inv_mid
    mine = g / (1.0 + jnp.exp(-g)) * (sums[1] * inv_mid)
    hidden_all[kv_me] = mine.astype(BF16)
    pending += exchange(
        "kv", kv_me, n_kv, lambda p: hidden_all.at[kv_me], hidden_all, send_e, recv_e
    )
    loads["down"].wait()
    await_arrivals(kv_me, n_kv, hidden_all, recv_e)
    for p in range(n_kv):
        hidden[p * seqs : (p + 1) * seqs, :units] = hidden_all[p].astype(F32)[:, :units]
    acc = jnp.zeros((rows, feats), F32)
    for start, size in tiles_of(padded, 256):
        acc = acc + dot(hidden[:, start : start + size].astype(BF16), down[start : start + size, :])
    lifted[tp_me] = acc.astype(BF16)
    pending += exchange("tp", tp_me, n_tp, lambda p: lifted.at[tp_me], lifted, send_f, recv_f)
    await_arrivals(tp_me, n_tp, lifted, recv_f)
    summed = lifted[0].astype(F32)
    for p in range(1, n_tp):
        summed = summed + lifted[p].astype(F32)
    out_ref[...] = (mid_f + summed).astype(BF16)
    for copy in pending:
        copy.wait_send()


def on_device(n_kv, n_tp, *args):
    (
        tokens,
        attn_gain,
        wq,
        wk,
        wv,
        wg,
        wc,
        dw,
        db,
        head_gain,
        key,
        value,
        decay,
        state,
        lengths,
        wo,
        mlp_gain,
        gate,
        up,
        down,
    ) = args
    row = lambda a: a.reshape(1, a.shape[0])
    operands = [
        tokens,
        row(attn_gain),
        wq,
        wk,
        wv,
        wg,
        wc,
        dw,
        row(db),
        row(head_gain),
        key,
        value,
        decay,
        state,
        lengths,
        wo,
        row(mlp_gain),
        gate,
        up,
        down,
    ]
    rows, feats = tokens.shape
    seqs, span, heads_here, key_dim = key.shape
    value_dim = value.shape[3]
    kw, vw = heads_here * key_dim, heads_here * value_dim
    units = gate.shape[1]
    rank = wc.shape[1]
    padded = (units + 2 + LANES - 1) // LANES * LANES
    cols = 2 * kw + 2 * vw + LANES
    vmem = pltpu.VMEM

    def copied(a):
        if a is lengths:
            return None
        if a is dw:
            return vmem((LANES, a.shape[1]), a.dtype)
        if a is down:
            return vmem((padded, a.shape[1]), a.dtype)
        return vmem(a.shape, a.dtype)

    scratch = [c for c in map(copied, operands) if c is not None]
    scratch += [
        vmem((rows, cols), F32),
        vmem((n_kv, seqs, cols), BF16),
        vmem((n_kv, seqs, cols), BF16),
        vmem((seqs, span, heads_here, key_dim), F32),
        vmem((seqs, heads_here, key_dim), F32),
        vmem((seqs, heads_here, key_dim), F32),
        vmem((seqs, heads_here, key_dim), F32),
        vmem((seqs, heads_here, value_dim), F32),
        vmem((seqs, vw), F32),
        vmem((rows, vw), F32),
        vmem((n_kv, seqs, vw), BF16),
        vmem((n_tp, rows, feats), BF16),
        vmem((rows, padded), F32),
        vmem((2, n_kv, seqs, padded), BF16),
        vmem((2, n_kv, seqs, padded), BF16),
        vmem((rows, padded), F32),
        vmem((n_kv, seqs, padded), BF16),
        vmem((n_tp, rows, feats), BF16),
    ]
    dma = pltpu.SemaphoreType.DMA
    scratch += [dma((19,))]
    scratch += [dma((n_kv,))] * 4
    scratch += [dma((n_tp,))] * 2
    scratch += [dma((2, n_kv))] * 2
    scratch += [dma((n_kv,))] * 2
    scratch += [dma((n_tp,))] * 2
    any_spec = pl.BlockSpec(memory_space=pl.ANY)
    in_specs = [
        pl.BlockSpec(memory_space=pltpu.SMEM) if a is lengths else any_spec for a in operands
    ]
    return pl.pallas_call(
        functools.partial(layer_kernel, n_kv, n_tp, feats * n_kv),
        out_shape=(
            jax.ShapeDtypeStruct((rows, feats), BF16),
            jax.ShapeDtypeStruct((seqs, heads_here, key_dim), BF16),
            jax.ShapeDtypeStruct((seqs, heads_here, value_dim), BF16),
        ),
        in_specs=in_specs,
        out_specs=(pl.BlockSpec(memory_space=pltpu.VMEM),) * 3,
        scratch_shapes=scratch,
        compiler_params=pltpu.CompilerParams(
            collective_id=0, has_side_effects=True, vmem_limit_bytes=60 * 1024 * 1024
        ),
        name="layer",
    )(*operands)


def solution(mesh):
    in_specs = (
        P(None, "kv"),
        P("kv"),
        P("kv", "tp"),
        P("kv", "tp"),
        P("kv", "tp"),
        P("kv", "tp"),
        P("kv", None),
        P(None, "tp"),
        P("tp"),
        P(),
        P("kv", None, "tp", None),
        P("kv", None, "tp", None),
        P("kv", None, "tp", None),
        P("kv", "tp", None, None),
        P("kv"),
        P("tp", "kv"),
        P("kv"),
        P("kv", "tp"),
        P("kv", "tp"),
        P("tp", "kv"),
    )
    out_specs = (P(None, "kv"), P("kv", "tp", None), P("kv", "tp", None))
    return jax.shard_map(
        functools.partial(on_device, mesh.shape["kv"], mesh.shape["tp"]),
        mesh=mesh,
        in_specs=in_specs,
        out_specs=out_specs,
        check_vma=False,
    )
```

```python
import functools

import jax
import jax.numpy as jnp
from jax import lax
from jax.experimental import pallas as pl
from jax.experimental.pallas import tpu as pltpu
from jax.sharding import PartitionSpec as P

EPS = 1e-06
GATE_TEMP = 16.0
FIRST_LOADS = 7
PARTS = 4
LANES = 128
F32 = jnp.float32
BF16 = jnp.bfloat16


def split_sum(column):
    high = column.astype(BF16).astype(F32)
    return high, column - high


def dot(left, right):
    return jnp.dot(left, right, preferred_element_type=F32)


def dot_t(left, right):
    return lax.dot_general(left, right, (((1,), (1,)), ((), ())), preferred_element_type=F32)


def tiles_of(total, step):
    return [(start, min(step, total - start)) for start in range(0, total, step)]


def pieces_of(units):
    each = units // PARTS // LANES * LANES
    head = units - (PARTS - 1) * each
    room = (head + 2 + LANES - 1) // LANES * LANES
    return [(0, head, room)] + [(head + k * each, each, each) for k in range(PARTS - 1)]


def copy_out(*refs):
    *arrays, sems = refs
    half = len(arrays) // 2
    copies = [
        pltpu.make_async_copy(arrays[k], arrays[half + k], sems.at[k]) for k in range(half)
    ]
    for copy in copies:
        copy.start()
    for copy in copies:
        copy.wait()


def layer_kernel(
    n_kv,
    n_tp,
    width,
    tokens_h,
    attn_gain_h,
    wq_h,
    wk_h,
    wv_h,
    wg_h,
    wc_h,
    dw_h,
    db_h,
    head_gain_h,
    key_h,
    value_h,
    decay_h,
    state_h,
    lengths_s,
    wo_h,
    mlp_gain_h,
    gate_h,
    up_h,
    down_h,
    out_ref,
    nk_ref,
    nv_ref,
    tokens,
    attn_gain,
    wq,
    wk,
    wv,
    wg,
    wc,
    dw,
    db,
    head_gain,
    key,
    value,
    decay,
    state,
    wo,
    mlp_gain,
    gate,
    up,
    down,
    proj,
    proj_send,
    proj_recv,
    keyed,
    total_exp,
    decayed3,
    keys3,
    values3,
    mixed,
    heads,
    heads_all,
    attended,
    accs,
    sends,
    recvs,
    hiddens,
    hiddens_all,
    lifted,
    load_sem,
    send_a,
    recv_a,
    send_b,
    recv_b,
    send_c,
    recv_c,
    send_d,
    recv_d,
    send_e,
    recv_e,
    send_f,
    recv_f,
):
    kv_me = lax.axis_index("kv")
    tp_me = lax.axis_index("tp")
    rows, feats = tokens.shape
    seqs, span, heads_here, key_dim = key.shape
    value_dim = value.shape[3]
    kw, vw = heads_here * key_dim, heads_here * value_dim
    rank = wc.shape[0]
    units = gate.shape[0]
    pieces = pieces_of(units)

    loads = {}
    pairs = [
        ("tokens", tokens_h, tokens),
        ("attn_gain", attn_gain_h, attn_gain),
        ("wc", wc_h, wc),
        ("wq", wq_h, wq),
        ("wk", wk_h, wk),
        ("wv", wv_h, wv),
        ("wg", wg_h, wg),
        ("decay", decay_h, decay),
        ("key", key_h, key),
        ("dw", dw_h, dw.at[pl.ds(0, rank)]),
        ("db", db_h, db),
        ("head_gain", head_gain_h, head_gain),
        ("state", state_h, state),
        ("value", value_h, value),
        ("wo", wo_h, wo),
        ("mlp_gain", mlp_gain_h, mlp_gain),
        ("gate", gate_h, gate),
        ("up", up_h, up),
        ("down", down_h, down),
    ]
    for place, (name, source, target) in enumerate(pairs):
        loads[name] = pltpu.make_async_copy(source, target, load_sem.at[place])
        if place < FIRST_LOADS:
            loads[name].start()

    def ready(*names):
        for name in names:
            loads.pop(name).wait()

    barrier = pltpu.get_barrier_semaphore()
    for off in range(1, n_kv):
        pl.semaphore_signal(
            barrier,
            inc=1,
            device_id={"kv": lax.rem(kv_me + off, n_kv)},
            device_id_type=pl.DeviceIdType.MESH,
        )
    for off in range(1, n_tp):
        pl.semaphore_signal(
            barrier,
            inc=1,
            device_id={"tp": lax.rem(tp_me + off, n_tp)},
            device_id_type=pl.DeviceIdType.MESH,
        )

    def exchange(axis, me, count, source, target, sent, arrived):
        started = []
        for off in range(count - 1, 0, -1):
            p = lax.rem(me + off, count)
            copy = pltpu.make_async_remote_copy(
                src_ref=source(p),
                dst_ref=target.at[me],
                send_sem=sent.at[off],
                recv_sem=arrived.at[me],
                device_id={axis: p},
                device_id_type=pl.DeviceIdType.MESH,
            )
            copy.start()
            started.append(copy)
        return started

    def await_arrivals(me, count, target, arrived):
        for off in range(1, count):
            p = lax.rem(me + off, count)
            pltpu.make_async_copy(target.at[p], target.at[p], arrived.at[p]).wait()

    pending = []

    base_misc = 2 * kw + 2 * vw
    ready(*("tokens", "attn_gain", "wc"))
    token_f = tokens[...].astype(F32)
    scaled = (token_f * attn_gain[...]).astype(BF16)
    proj[:, base_misc:] = jnp.zeros((rows, LANES), F32)
    proj[:, base_misc : base_misc + rank] = dot_t(scaled, wc[...])
    high, low = split_sum(jnp.sum(token_f * token_f, axis=1, keepdims=True))
    proj[:, base_misc + rank : base_misc + rank + 1] = high
    proj[:, base_misc + rank + 1 : base_misc + rank + 2] = low
    base = 0
    for name, weight in (("wq", wq), ("wk", wk), ("wv", wv), ("wg", wg)):
        ready(name)
        if name == "wg":
            for late in list(loads.values()):
                late.start()
        for start, size in tiles_of(weight.shape[1], 256):
            proj[:, base + start : base + start + size] = dot(
                scaled, weight[:, start : start + size]
            )
        base += weight.shape[1]
    for p in range(n_kv):
        proj_send[p] = proj[p * seqs : (p + 1) * seqs, :].astype(BF16)
    pl.semaphore_wait(barrier, n_kv + n_tp - 2)
    pending += exchange("kv", kv_me, n_kv, lambda p: proj_send.at[p], proj_recv, send_a, recv_a)
    proj_recv[kv_me] = proj_send[kv_me]

    dw[rank:, :] = jnp.zeros((dw.shape[0] - rank, dw.shape[1]), BF16)
    ready("decay")
    ready("key")
    positions = lax.broadcasted_iota(jnp.int32, (span, heads_here, key_dim), 0)
    for b in range(seqs):
        live = positions < lengths_s[b]
        kept = jnp.where(live, decay[b], 0.0)
        suffix = kept
        step = 1
        while step < span:
            suffix = suffix + jnp.concatenate(
                [suffix[step:], jnp.zeros((step, heads_here, key_dim), F32)], axis=0
            )
            step *= 2
        total_exp[b] = jnp.exp(suffix[0])
        later = jnp.concatenate([suffix[1:], jnp.zeros((1, heads_here, key_dim), F32)], axis=0)
        keyed[b] = jnp.where(live, key[b].astype(F32) * jnp.exp(later), 0.0)
    ready(*("dw", "db", "head_gain", "state", "value"))

    await_arrivals(kv_me, n_kv, proj_recv, recv_a)
    total = proj_recv[0].astype(F32)
    for p in range(1, n_kv):
        total = total + proj_recv[p].astype(F32)
    misc = total[:, base_misc:]
    squares = misc[:, rank : rank + 1] + misc[:, rank + 1 : rank + 2]
    inv_rms = lax.rsqrt(squares / width + EPS)
    queries = (total[:, :kw] * inv_rms * key_dim ** (-0.5)).astype(BF16).astype(F32)
    new_keys = (total[:, kw : 2 * kw] * inv_rms).astype(BF16).astype(F32)
    new_values = (total[:, 2 * kw : 2 * kw + vw] * inv_rms).astype(BF16).astype(F32)
    out_gate = (total[:, 2 * kw + vw : base_misc] * inv_rms).astype(BF16).astype(F32)
    code = (misc * inv_rms).astype(BF16)
    pre_gate = dot(code, dw[...]) + db[...]
    new_decay = (jnp.minimum(pre_gate, 0.0) - jnp.log1p(jnp.exp(-jnp.abs(pre_gate)))) / GATE_TEMP
    decayed = queries * jnp.exp(new_decay)
    for b in range(seqs):
        for h in range(heads_here):
            k_cols = slice(h * key_dim, (h + 1) * key_dim)
            v_cols = slice(h * value_dim, (h + 1) * value_dim)
            decayed3[b, h : h + 1, :] = decayed[b : b + 1, k_cols]
            keys3[b, h : h + 1, :] = new_keys[b : b + 1, k_cols]
            values3[b, h : h + 1, :] = new_values[b : b + 1, v_cols]
    nk_ref[...] = keys3[...].astype(BF16)
    nv_ref[...] = values3[...].astype(BF16)
    for b in range(seqs):
        d = decayed3[b]
        scores = jnp.sum(keyed[b] * d[None], axis=-1, keepdims=True)
        scores = scores.astype(BF16).astype(F32)
        within = jnp.sum(scores * value[b].astype(F32), axis=0)
        into_state = jnp.transpose(
            jnp.concatenate(
                [d * total_exp[b], jnp.zeros((8 - heads_here, key_dim), F32)], axis=0
            )
        )
        for h in range(heads_here):
            carried = jnp.sum(into_state[:, h : h + 1] * state[b, h], axis=0, keepdims=True)
            mixed[b : b + 1, h * value_dim : (h + 1) * value_dim] = carried + within[h : h + 1]
    for h in range(heads_here):
        k_cols = slice(h * key_dim, (h + 1) * key_dim)
        v_cols = slice(h * value_dim, (h + 1) * value_dim)
        own = jnp.sum(queries[:, k_cols] * new_keys[:, k_cols], axis=-1, keepdims=True)
        full = mixed[:, v_cols] + own * new_values[:, v_cols]
        norm = lax.rsqrt(jnp.mean(full * full, axis=-1, keepdims=True) + EPS)
        g = out_gate[:, v_cols]
        mixed[:, v_cols] = full * norm * head_gain[...] * (g / (1.0 + jnp.exp(-g)))
    heads_all[kv_me] = mixed[...].astype(BF16)
    pending += exchange(
        "kv", kv_me, n_kv, lambda p: heads_all.at[kv_me], heads_all, send_b, recv_b
    )

    ready("wo")
    ready("mlp_gain")
    await_arrivals(kv_me, n_kv, heads_all, recv_b)
    for p in range(n_kv):
        heads[p * seqs : (p + 1) * seqs, :] = heads_all[p].astype(F32)
    attended[tp_me] = dot(heads[...].astype(BF16), wo[...]).astype(BF16)
    pending += exchange(
        "tp", tp_me, n_tp, lambda p: attended.at[tp_me], attended, send_c, recv_c
    )
    ready("gate")
    await_arrivals(tp_me, n_tp, attended, recv_c)
    summed = attended[0].astype(F32)
    for p in range(1, n_tp):
        summed = summed + attended[p].astype(F32)
    mid_f = (token_f + summed).astype(BF16).astype(F32)
    scaled_mid = (mid_f * mlp_gain[...]).astype(BF16)

    ready("up")
    for part, (first, size, span_cols) in enumerate(pieces):
        mlp_acc = accs[part]
        for base, weight in ((0, gate), (span_cols, up)):
            if size < span_cols:
                mlp_acc[:, base + span_cols - LANES : base + span_cols] = jnp.zeros(
                    (rows, LANES), F32
                )
            for start, count in tiles_of(size, 256):
                mlp_acc[:, base + start : base + start + count] = dot_t(
                    scaled_mid, weight[first + start : first + start + count, :]
                )
        if part == 0:
            high, low = split_sum(jnp.sum(mid_f * mid_f, axis=1, keepdims=True))
            mlp_acc[:, size : size + 1] = high
            mlp_acc[:, size + 1 : size + 2] = low
        for p in range(n_kv):
            sends[part][p] = mlp_acc[p * seqs : (p + 1) * seqs, :].astype(BF16)
        pending += exchange(
            "kv",
            kv_me,
            n_kv,
            lambda p, part=part: sends[part].at[p],
            recvs[part],
            send_d.at[part],
            recv_d.at[part],
        )
        recvs[part][kv_me] = sends[part][kv_me]
    for part, (first, size, span_cols) in enumerate(pieces):
        await_arrivals(kv_me, n_kv, recvs[part], recv_d.at[part])
        total = recvs[part][0].astype(F32)
        for p in range(1, n_kv):
            total = total + recvs[part][p].astype(F32)
        if part == 0:
            squares = total[:, size : size + 1] + total[:, size + 1 : size + 2]
            inv_mid = lax.rsqrt(squares / width + EPS)
        g = total[:, :span_cols] * inv_mid
        mine = g / (1.0 + jnp.exp(-g)) * (total[:, span_cols:] * inv_mid)
        hiddens_all[part][kv_me] = mine.astype(BF16)
        pending += exchange(
            "kv",
            kv_me,
            n_kv,
            lambda p, part=part: hiddens_all[part].at[kv_me],
            hiddens_all[part],
            send_e.at[part],
            recv_e.at[part],
        )
    ready("down")
    acc = jnp.zeros((rows, feats), F32)
    for part, (first, size, span_cols) in enumerate(pieces):
        await_arrivals(kv_me, n_kv, hiddens_all[part], recv_e.at[part])
        hidden = hiddens[part]
        for p in range(n_kv):
            hidden[p * seqs : (p + 1) * seqs, :] = hiddens_all[part][p].astype(F32)
        if size < span_cols:
            lane = lax.broadcasted_iota(jnp.int32, (rows, span_cols), 1)
            whole = jnp.where(lane < size, hidden[...], 0.0).astype(BF16)
        else:
            whole = hidden[...].astype(BF16)
        acc = acc + dot(whole, down[first : first + span_cols, :])
    lifted[tp_me] = acc.astype(BF16)
    pending += exchange("tp", tp_me, n_tp, lambda p: lifted.at[tp_me], lifted, send_f, recv_f)
    await_arrivals(tp_me, n_tp, lifted, recv_f)
    summed = lifted[0].astype(F32)
    for p in range(1, n_tp):
        summed = summed + lifted[p].astype(F32)
    out_ref[...] = (mid_f + summed).astype(BF16)
    for copy in pending:
        copy.wait_send()


def on_device(n_kv, n_tp, *args):
    (
        tokens,
        attn_gain,
        wq,
        wk,
        wv,
        wg,
        wc,
        dw,
        db,
        head_gain,
        key,
        value,
        decay,
        state,
        lengths,
        wo,
        mlp_gain,
        gate,
        up,
        down,
    ) = args
    row = lambda a: a.reshape(1, a.shape[0])
    operands = [
        tokens,
        row(attn_gain),
        wq,
        wk,
        wv,
        wg,
        wc.T,
        dw,
        row(db),
        row(head_gain),
        key,
        value,
        decay,
        state,
        lengths,
        wo,
        row(mlp_gain),
        gate.T,
        up.T,
        down,
    ]
    rows, feats = tokens.shape
    seqs, span, heads_here, key_dim = key.shape
    value_dim = value.shape[3]
    kw, vw = heads_here * key_dim, heads_here * value_dim
    units = gate.shape[1]
    rank = wc.shape[1]
    widths = [piece[2] for piece in pieces_of(units)]
    cols = 2 * kw + 2 * vw + LANES
    vmem = pltpu.VMEM

    def copied(a):
        if a is lengths:
            return None
        if a is dw:
            return vmem((LANES, a.shape[1]), a.dtype)
        return vmem(a.shape, a.dtype)

    scratch = [c for c in map(copied, operands) if c is not None]
    scratch += [
        vmem((rows, cols), F32),
        vmem((n_kv, seqs, cols), BF16),
        vmem((n_kv, seqs, cols), BF16),
        vmem((seqs, span, heads_here, key_dim), F32),
        vmem((seqs, heads_here, key_dim), F32),
        vmem((seqs, heads_here, key_dim), F32),
        vmem((seqs, heads_here, key_dim), F32),
        vmem((seqs, heads_here, value_dim), F32),
        vmem((seqs, vw), F32),
        vmem((rows, vw), F32),
        vmem((n_kv, seqs, vw), BF16),
        vmem((n_tp, rows, feats), BF16),
        [vmem((rows, 2 * w), F32) for w in widths],
        [vmem((n_kv, seqs, 2 * w), BF16) for w in widths],
        [vmem((n_kv, seqs, 2 * w), BF16) for w in widths],
        [vmem((rows, w), F32) for w in widths],
        [vmem((n_kv, seqs, w), BF16) for w in widths],
        vmem((n_tp, rows, feats), BF16),
    ]
    dma = pltpu.SemaphoreType.DMA
    scratch += [dma((19,))]
    scratch += [dma((n_kv,))] * 4
    scratch += [dma((n_tp,))] * 2
    scratch += [dma((PARTS, n_kv))] * 4
    scratch += [dma((n_tp,))] * 2
    hbm_spec = pl.BlockSpec(memory_space=pltpu.HBM)
    in_specs = [
        pl.BlockSpec(memory_space=pltpu.SMEM) if a is lengths else hbm_spec for a in operands
    ]
    shapes = ((rows, feats), (seqs, heads_here, key_dim), (seqs, heads_here, value_dim))
    results = pl.pallas_call(
        functools.partial(layer_kernel, n_kv, n_tp, feats * n_kv),
        out_shape=tuple(vmem(shape, BF16) for shape in shapes),
        in_specs=in_specs,
        out_specs=(pl.BlockSpec(memory_space=pltpu.VMEM),) * 3,
        scratch_shapes=scratch,
        compiler_params=pltpu.CompilerParams(
            collective_id=0, has_side_effects=True, vmem_limit_bytes=66900000
        ),
        name="layer",
    )(*operands)
    local = (pl.BlockSpec(memory_space=pl.ANY),) * 3
    return pl.pallas_call(
        copy_out,
        out_shape=tuple(jax.ShapeDtypeStruct(shape, BF16) for shape in shapes),
        in_specs=local,
        out_specs=local,
        scratch_shapes=[dma((3,))],
        name="results",
    )(*results)


def solution(mesh):
    in_specs = (
        P(None, "kv"),
        P("kv"),
        P("kv", "tp"),
        P("kv", "tp"),
        P("kv", "tp"),
        P("kv", "tp"),
        P("kv", None),
        P(None, "tp"),
        P("tp"),
        P(),
        P("kv", None, "tp", None),
        P("kv", None, "tp", None),
        P("kv", None, "tp", None),
        P("kv", "tp", None, None),
        P("kv"),
        P("tp", "kv"),
        P("kv"),
        P("kv", "tp"),
        P("kv", "tp"),
        P("tp", "kv"),
    )
    out_specs = (P(None, "kv"), P("kv", "tp", None), P("kv", "tp", None))
    return jax.shard_map(
        functools.partial(on_device, mesh.shape["kv"], mesh.shape["tp"]),
        mesh=mesh,
        in_specs=in_specs,
        out_specs=out_specs,
        check_vma=False,
    )
```
